32 devices in a mesh: rep: 4 (over z), fs: 4 (over y, x), tp: 2 (over core).
Axes of the slice: x: 2, y: 2, z: 4, core: 2. Of those that a mesh axis runs over, the one named last changes fastest.
Arguments:
- skip_stream_entry: bfloat16 [4096, 2048], P(('rep', 'fs')), may hold values from -6 to 6
- sequence_blender_factor: float32 [2048], replicated, may hold values from 0.1 to 1.9
- product_projector: float32 [2048, 1024], P('fs', 'tp'), may hold values from -0.125 to 0.125
- product_side_factors: float32 [1024], P('tp'), may hold values from 0.3 to 3
- placewise_projector: float32 [2048, 1024], P('fs', 'tp'), may hold values from -0.125 to 0.125
- placewise_entry_factors: float32 [1024], P('tp'), may hold values from 0.7 to 11.2, as said below
- placewise_rescale_factor: float32 [1024], P('tp'), may hold values from 0.1 to 1.9
- place_cluster_operator: bfloat16 [8, 128, 128], replicated, may hold values from -0.5 to 0.5
- placewise_offset_vector: float32 [8, 128], replicated, may hold values from 0.1 to 1.9
- blender_result_projector: float32 [1024, 2048], P('tp', 'fs'), may hold values from -0.1875 to 0.1875
- blender_result_factors: float32 [2048], P('fs'), may hold values from 0.3 to 3
- feedforward_norm_factor: float32 [2048], replicated, may hold values from 0.1 to 1.9
- switch_projector: float32 [2048, 2816], P('fs', 'tp'), may hold values from -0.125 to 0.125
- switch_factors: float32 [2816], P('tp'), may hold values from 0.3 to 3
- expand_projector: float32 [2048, 2816], P('fs', 'tp'), may hold values from -0.125 to 0.125
- expand_factors: float32 [2816], P('tp'), may hold values from 0.3 to 3
- contract_projector: float32 [2816, 2048], P('tp', 'fs'), may hold values from -0.109375 to 0.109375
- contract_factors: float32 [2048], P('fs'), may hold values from 0.3 to 3
Outputs:
- result: bfloat16 [4096, 2048], P(('rep', 'fs'), 'tp')
The draws below stay inside these ranges and needn't reach their ends.
Inputs may be any that keep to these rules, and one draw needn't show every extreme that they name: `placewise_entry_factors`: positive column scales.
All inputs are finite; a program needn't handle non-finite values.
Results may differ from the reference program's by a relative error of at most 0.023.
Values may be sent and summed in bfloat16 or wider, within the bound.
A program may use at most 64 MiB of HBM per device.

```python
import math
import jax
import jax.numpy as jnp
from jax import lax

EMBED_DIMENSION = 2048
BLENDER_FEATURES = 1024
GROUP_DIM = 128
BLOCK = 128
FF = 2816
SHARED_SEQ_STEPS = 256
GROUPS = 8
TOKENS = 4096
N_REP = 4
N_FS = 4
N_TP = 2


def draw_placewise_entry_factors(key, part):
    column_pos = jnp.arange(BLENDER_FEATURES, dtype=jnp.float32) / (BLENDER_FEATURES - 1)
    rising = jnp.exp(jnp.log(4.0) * column_pos)
    rough_part = jnp.exp(jax.random.uniform(key, (BLENDER_FEATURES,), jnp.float32, jnp.log(0.7), jnp.log(1.4)))
    return rising * rough_part


def levels(stream_key, extent, cuts, least, largest):
    level, own = 1.0, jax.random.fold_in(stream_key, 6)
    for position, shards_of in cuts:
        heights = jnp.exp(jax.random.uniform(jax.random.fold_in(own, position), (shards_of,), jnp.float32, least / len(cuts), largest / len(cuts)))
        level = level * jnp.repeat(heights, extent[position] // shards_of).reshape([-1 if axis == position else 1 for axis in range(len(extent))])
    return level


def bell_draw(rng, dims, scale, reach, split=(), kind=jnp.bfloat16):
    drawn = jax.random.normal(rng, dims, jnp.float32) * scale
    if len(split) > 0:
        drawn = levels(rng, dims, split, -0.22, 0.18) * drawn
    return jnp.clip(drawn, min=-reach, max=reach).astype(kind)


def setup_inputs(seed: int = 0) -> dict:
    key_of = jax.random.split(jax.random.key(seed), 19)
    skip_stream_entry = bell_draw(key_of[0], (TOKENS, EMBED_DIMENSION), 1.0, 6.0, ((0, 16),))
    sequence_blender_factor = jnp.clip(1.0 + 0.18 * jax.random.normal(key_of[1], (EMBED_DIMENSION,), jnp.float32), 0.1, 1.9)
    product_projector = bell_draw(key_of[2], (EMBED_DIMENSION, BLENDER_FEATURES), EMBED_DIMENSION ** -0.5, 0.125, ((0, 4), (1, 2)), jnp.float32)
    product_side_factors = jnp.clip(jnp.exp(math.log(3.0) - 2.3025851 * jax.random.uniform(key_of[3], (BLENDER_FEATURES,), jnp.float32) ** levels(key_of[3], (BLENDER_FEATURES,), ((0, 2),), -0.2, 0.2)), 0.3, 3.0)
    placewise_projector = bell_draw(key_of[4], (EMBED_DIMENSION, BLENDER_FEATURES), EMBED_DIMENSION ** -0.5, 0.125, ((0, 4), (1, 2)), jnp.float32)
    placewise_entry_factors = draw_placewise_entry_factors(jax.random.fold_in(key_of[18], 71), 0)
    placewise_rescale_factor = jnp.clip(1.0 + 0.18 * jax.random.normal(key_of[6], (BLENDER_FEATURES,), jnp.float32), 0.1, 1.9)
    place_cluster_operator = bell_draw(key_of[7], (GROUPS, BLOCK, BLOCK), BLOCK ** -0.5, 0.5)
    placewise_offset_vector = jnp.clip(1.0 + 0.18 * jax.random.normal(key_of[8], (GROUPS, BLOCK), jnp.float32), 0.1, 1.9)
    blender_result_projector = bell_draw(key_of[9], (BLENDER_FEATURES, EMBED_DIMENSION), BLENDER_FEATURES ** -0.5, 0.1875, ((0, 2), (1, 4)), jnp.float32)
    blender_result_factors = jnp.clip(jnp.exp(math.log(3.0) - 2.3025851 * jax.random.uniform(key_of[10], (EMBED_DIMENSION,), jnp.float32) ** levels(key_of[10], (EMBED_DIMENSION,), ((0, 4),), -0.2, 0.2)), 0.3, 3.0)
    feedforward_norm_factor = jnp.clip(1.0 + 0.18 * jax.random.normal(key_of[11], (EMBED_DIMENSION,), jnp.float32), 0.1, 1.9)
    switch_projector = bell_draw(key_of[12], (EMBED_DIMENSION, FF), EMBED_DIMENSION ** -0.5, 0.125, ((0, 4), (1, 2)), jnp.float32)
    switch_factors = jnp.clip(jnp.exp(math.log(3.0) - 2.3025851 * jax.random.uniform(key_of[13], (FF,), jnp.float32) ** levels(key_of[13], (FF,), ((0, 2),), -0.2, 0.2)), 0.3, 3.0)
    expand_projector = bell_draw(key_of[14], (EMBED_DIMENSION, FF), EMBED_DIMENSION ** -0.5, 0.125, ((0, 4), (1, 2)), jnp.float32)
    expand_factors = jnp.clip(jnp.exp(math.log(3.0) - 2.3025851 * jax.random.uniform(key_of[15], (FF,), jnp.float32) ** levels(key_of[15], (FF,), ((0, 2),), -0.2, 0.2)), 0.3, 3.0)
    contract_projector = bell_draw(key_of[16], (FF, EMBED_DIMENSION), FF ** -0.5, 0.109375, ((0, 2), (1, 4)), jnp.float32)
    contract_factors = jnp.clip(jnp.exp(math.log(3.0) - 2.3025851 * jax.random.uniform(key_of[17], (EMBED_DIMENSION,), jnp.float32) ** levels(key_of[17], (EMBED_DIMENSION,), ((0, 4),), -0.2, 0.2)), 0.3, 3.0)
    return dict(skip_stream_entry=skip_stream_entry, sequence_blender_factor=sequence_blender_factor, product_projector=product_projector, product_side_factors=product_side_factors, placewise_projector=placewise_projector, placewise_entry_factors=placewise_entry_factors, placewise_rescale_factor=placewise_rescale_factor, place_cluster_operator=place_cluster_operator, placewise_offset_vector=placewise_offset_vector, blender_result_projector=blender_result_projector, blender_result_factors=blender_result_factors, feedforward_norm_factor=feedforward_norm_factor, switch_projector=switch_projector, switch_factors=switch_factors, expand_projector=expand_projector, expand_factors=expand_factors, contract_projector=contract_projector, contract_factors=contract_factors)


epsilon = 1e-06

def normalize(values, gain):
    return values * lax.rsqrt(lax.optimization_barrier(jnp.mean(values * values, axis=-1, keepdims=True)) + epsilon) * gain

def shard_total(activations, weight, scale):
    shards = activations.astype(jnp.float32).reshape(activations.shape[0], N_TP, -1)
    pieces = weight.astype(jnp.float32).reshape(N_TP, -1, weight.shape[1])
    partial_value = jnp.einsum('tkc,kcd->ktd', shards, pieces) * scale
    rounded = lax.optimization_barrier(partial_value.astype(jnp.bfloat16))
    return lax.optimization_barrier(jnp.sum(rounded.astype(jnp.float32), axis=0))

def reference(skip_stream_entry, sequence_blender_factor, product_projector, product_side_factors, placewise_projector, placewise_entry_factors, placewise_rescale_factor, place_cluster_operator, placewise_offset_vector, blender_result_projector, blender_result_factors, feedforward_norm_factor, switch_projector, switch_factors, expand_projector, expand_factors, contract_projector, contract_factors):
    product_lowered = product_projector.astype(jnp.bfloat16)
    spread_low = placewise_projector.astype(jnp.bfloat16)
    mix_out_low = blender_result_projector.astype(jnp.bfloat16)
    gate_low = switch_projector.astype(jnp.bfloat16)
    up_low = expand_projector.astype(jnp.bfloat16)
    down_low = contract_projector.astype(jnp.bfloat16)
    causal = jnp.tril(jnp.ones((BLOCK, BLOCK), dtype=bool))
    masked = jnp.where(causal[None], place_cluster_operator, jnp.zeros_like(place_cluster_operator)).astype(jnp.float32)

    def layer(rows):
        standardized_stream = normalize(rows.astype(jnp.float32), sequence_blender_factor).astype(jnp.bfloat16)
        product_portion = jax.nn.gelu(jnp.dot(standardized_stream, product_lowered, preferred_element_type=jnp.float32) * product_side_factors)
        spread = jax.nn.gelu(jnp.dot(standardized_stream, spread_low, preferred_element_type=jnp.float32) * placewise_entry_factors)
        spread_normed = normalize(spread, placewise_rescale_factor).astype(jnp.bfloat16)
        blocks = spread_normed.astype(jnp.float32).reshape(SHARED_SEQ_STEPS // BLOCK, BLOCK, GROUPS, GROUP_DIM)
        blended_sequence = jnp.einsum('gts,nsgc->ntgc', masked, blocks, precision=lax.Precision.HIGHEST)
        blended_sequence = blended_sequence + placewise_offset_vector.T[None, :, :, None]
        switched_inner = (product_portion * blended_sequence.reshape(SHARED_SEQ_STEPS, BLENDER_FEATURES)).astype(jnp.bfloat16)
        stream = (rows.astype(jnp.float32) + shard_total(switched_inner, mix_out_low, blender_result_factors)).astype(jnp.bfloat16)
        ffn_normed = normalize(stream.astype(jnp.float32), feedforward_norm_factor).astype(jnp.bfloat16)
        gate = jnp.dot(ffn_normed, gate_low, preferred_element_type=jnp.float32) * switch_factors
        upper = jnp.dot(ffn_normed, up_low, preferred_element_type=jnp.float32) * expand_factors
        active = (jax.nn.silu(gate) * upper).astype(jnp.bfloat16)
        return (stream.astype(jnp.float32) + shard_total(active, down_low, contract_factors)).astype(jnp.bfloat16)
    grouped = skip_stream_entry.reshape(N_REP * N_FS, SHARED_SEQ_STEPS, EMBED_DIMENSION)
    return lax.map(layer, grouped).reshape(TOKENS, EMBED_DIMENSION)
```

```python
import jax
import jax.numpy as jnp
from jax import lax
from jax.sharding import PartitionSpec as P

BLENDER_FEATURES = 1024
GROUP_DIM = 128
BLOCK = 128


epsilon = 1e-06


def normalize(values, gain):
    return values * lax.rsqrt(jnp.mean(values * values, axis=-1, keepdims=True) + epsilon) * gain


def on_device(
    skip_stream_entry,
    sequence_blender_factor,
    product_projector,
    product_side_factors,
    placewise_projector,
    placewise_entry_factors,
    placewise_rescale_factor,
    place_cluster_operator,
    placewise_offset_vector,
    blender_result_projector,
    blender_result_factors,
    feedforward_norm_factor,
    switch_projector,
    switch_factors,
    expand_projector,
    expand_factors,
    contract_projector,
    contract_factors,
):
    rep = lax.axis_size("rep")
    tp = lax.axis_size("tp")
    rep_index = lax.axis_index("rep")
    tp_index = lax.axis_index("tp")
    group = ("rep", "tp")
    steps, embed = skip_stream_entry.shape
    own_steps = steps // tp
    own_features = embed // tp
    channels = product_projector.shape[1] // rep
    hidden = switch_projector.shape[1] // rep

    def part(values, size, dim):
        return lax.dynamic_slice_in_dim(values, rep_index * size, size, dim)

    def gathered(first, second, out, size):
        return lax.all_gather(
            jnp.concatenate(
                (
                    part(first, size, 1).astype(jnp.bfloat16),
                    part(second, size, 1).astype(jnp.bfloat16),
                    part(out, size, 0).astype(jnp.bfloat16).T,
                ),
                axis=1,
            ),
            "fs",
            axis=0,
            tiled=True,
        )

    own_entry = lax.dynamic_slice_in_dim(skip_stream_entry, tp_index * own_steps, own_steps, 0)
    normed = lax.all_gather(
        normalize(own_entry.astype(jnp.float32), sequence_blender_factor).astype(jnp.bfloat16),
        group,
        axis=0,
        tiled=True,
    )
    mixer_weights = gathered(
        product_projector, placewise_projector, blender_result_projector, channels
    )
    out_scales = lax.all_gather(
        jnp.stack((blender_result_factors, contract_factors)), "fs", axis=1, tiled=True
    )
    ffn_weights = gathered(switch_projector, expand_projector, contract_projector, hidden)

    tokens = normed.shape[0]
    plain = jnp.dot(normed, mixer_weights[:, : 2 * channels], preferred_element_type=jnp.float32)
    carrier = jax.nn.gelu(plain[:, :channels] * part(product_side_factors, channels, 0))
    spread = jax.nn.gelu(plain[:, channels:] * part(placewise_entry_factors, channels, 0))
    squares = lax.psum(jnp.sum(spread * spread, axis=1), group)
    factor = lax.rsqrt(squares / BLENDER_FEATURES + epsilon)
    spread_normed = (
        spread * factor[:, None] * part(placewise_rescale_factor, channels, 0)
    ).astype(jnp.bfloat16)
    span = min(channels, GROUP_DIM)
    count = max(1, channels // GROUP_DIM)
    first_group = (tp_index * rep + rep_index) * channels // GROUP_DIM
    causal = jnp.tril(jnp.ones((BLOCK, BLOCK), dtype=bool))
    local_weight = lax.dynamic_slice_in_dim(place_cluster_operator, first_group, count, 0)
    local_weight = jnp.where(causal[None], local_weight, jnp.zeros_like(local_weight))
    local_bias = lax.dynamic_slice_in_dim(placewise_offset_vector, first_group, count, 0)
    blocks = spread_normed.reshape(tokens // BLOCK, BLOCK, count, span)
    mixed = jnp.einsum("gts,nsgc->ntgc", local_weight, blocks, preferred_element_type=jnp.float32)
    mixed = mixed + local_bias.T[None, :, :, None]
    gated = (carrier * mixed.reshape(tokens, channels)).astype(jnp.bfloat16)

    def projected(values, weights, scales):
        return (
            lax.dot_general(
                values, weights, (((1,), (1,)), ((), ())), preferred_element_type=jnp.float32
            )
            * scales
        ).astype(jnp.bfloat16)

    mix_total = lax.psum_scatter(
        projected(gated, mixer_weights[:, 2 * channels :], out_scales[0]),
        group,
        scatter_dimension=0,
        tiled=True,
    )
    stream = (own_entry.astype(jnp.float32) + mix_total.astype(jnp.float32)).astype(jnp.bfloat16)
    stream_all = lax.all_gather(stream, group, axis=0, tiled=True)
    ffn_normed = normalize(stream_all.astype(jnp.float32), feedforward_norm_factor).astype(
        jnp.bfloat16
    )
    plain = jnp.dot(ffn_normed, ffn_weights[:, : 2 * hidden], preferred_element_type=jnp.float32)
    active = (
        jax.nn.silu(plain[:, :hidden] * part(switch_factors, hidden, 0))
        * (plain[:, hidden:] * part(expand_factors, hidden, 0))
    ).astype(jnp.bfloat16)
    ffn_terms = projected(active, ffn_weights[:, 2 * hidden :], out_scales[1])
    ffn_terms = ffn_terms.reshape(rep, steps, tp, own_features).transpose(0, 2, 1, 3)
    ffn_total = lax.psum_scatter(
        ffn_terms.reshape(rep * tp * steps, own_features), group, scatter_dimension=0, tiled=True
    )
    own_stream = lax.dynamic_slice(
        stream_all, (rep_index * steps, tp_index * own_features), (steps, own_features)
    )
    return (own_stream.astype(jnp.float32) + ffn_total.astype(jnp.float32)).astype(jnp.bfloat16)


def solution(mesh):
    return jax.shard_map(
        on_device,
        mesh=mesh,
        in_specs=(
            P(("rep", "fs"), None),
            P(),
            P("fs", "tp"),
            P("tp"),
            P("fs", "tp"),
            P("tp"),
            P("tp"),
            P(),
            P(),
            P("tp", "fs"),
            P("fs"),
            P(),
            P("fs", "tp"),
            P("tp"),
            P("fs", "tp"),
            P("tp"),
            P("tp", "fs"),
            P("fs"),
        ),
        out_specs=P(("rep", "fs"), "tp"),
        check_vma=False,
    )
```

```python
import functools

import jax
import jax.numpy as jnp
from jax import lax
from jax.experimental import pallas as pl
from jax.experimental.pallas import tpu as pltpu
from jax.sharding import PartitionSpec as P

BLENDER_FEATURES = 1024
GROUP_DIM = 128
BLOCK = 128


epsilon = 1e-06


def normalize(values, gain):
    return values * lax.rsqrt(jnp.mean(values * values, axis=-1, keepdims=True) + epsilon) * gain


def with_collectives(
    skip_stream_entry,
    sequence_blender_factor,
    product_projector,
    product_side_factors,
    placewise_projector,
    placewise_entry_factors,
    placewise_rescale_factor,
    place_cluster_operator,
    placewise_offset_vector,
    blender_result_projector,
    blender_result_factors,
    feedforward_norm_factor,
    switch_projector,
    switch_factors,
    expand_projector,
    expand_factors,
    contract_projector,
    contract_factors,
):
    rep = lax.axis_size("rep")
    tp = lax.axis_size("tp")
    rep_index = lax.axis_index("rep")
    tp_index = lax.axis_index("tp")
    group = ("rep", "tp")
    steps, embed = skip_stream_entry.shape
    own_steps = steps // tp
    own_features = embed // tp
    channels = product_projector.shape[1] // rep
    hidden = switch_projector.shape[1] // rep

    def part(values, size, dim):
        return lax.dynamic_slice_in_dim(values, rep_index * size, size, dim)

    def gathered(first, second, out, size):
        return lax.all_gather(
            jnp.concatenate(
                (
                    part(first, size, 1).astype(jnp.bfloat16),
                    part(second, size, 1).astype(jnp.bfloat16),
                    part(out, size, 0).astype(jnp.bfloat16).T,
                ),
                axis=1,
            ),
            "fs",
            axis=0,
            tiled=True,
        )

    own_entry = lax.dynamic_slice_in_dim(skip_stream_entry, tp_index * own_steps, own_steps, 0)
    normed = lax.all_gather(
        normalize(own_entry.astype(jnp.float32), sequence_blender_factor).astype(jnp.bfloat16),
        group,
        axis=0,
        tiled=True,
    )
    mixer_weights = gathered(
        product_projector, placewise_projector, blender_result_projector, channels
    )
    out_scales = lax.all_gather(
        jnp.stack((blender_result_factors, contract_factors)), "fs", axis=1, tiled=True
    )
    ffn_weights = gathered(switch_projector, expand_projector, contract_projector, hidden)

    tokens = normed.shape[0]
    plain = jnp.dot(normed, mixer_weights[:, : 2 * channels], preferred_element_type=jnp.float32)
    carrier = jax.nn.gelu(plain[:, :channels] * part(product_side_factors, channels, 0))
    spread = jax.nn.gelu(plain[:, channels:] * part(placewise_entry_factors, channels, 0))
    squares = lax.psum(jnp.sum(spread * spread, axis=1), group)
    factor = lax.rsqrt(squares / BLENDER_FEATURES + epsilon)
    spread_normed = (
        spread * factor[:, None] * part(placewise_rescale_factor, channels, 0)
    ).astype(jnp.bfloat16)
    span = min(channels, GROUP_DIM)
    count = max(1, channels // GROUP_DIM)
    first_group = (tp_index * rep + rep_index) * channels // GROUP_DIM
    causal = jnp.tril(jnp.ones((BLOCK, BLOCK), dtype=bool))
    local_weight = lax.dynamic_slice_in_dim(place_cluster_operator, first_group, count, 0)
    local_weight = jnp.where(causal[None], local_weight, jnp.zeros_like(local_weight))
    local_bias = lax.dynamic_slice_in_dim(placewise_offset_vector, first_group, count, 0)
    blocks = spread_normed.reshape(tokens // BLOCK, BLOCK, count, span)
    mixed = jnp.einsum("gts,nsgc->ntgc", local_weight, blocks, preferred_element_type=jnp.float32)
    mixed = mixed + local_bias.T[None, :, :, None]
    gated = (carrier * mixed.reshape(tokens, channels)).astype(jnp.bfloat16)

    def projected(values, weights, scales):
        return (
            lax.dot_general(
                values, weights, (((1,), (1,)), ((), ())), preferred_element_type=jnp.float32
            )
            * scales
        ).astype(jnp.bfloat16)

    mix_total = lax.psum_scatter(
        projected(gated, mixer_weights[:, 2 * channels :], out_scales[0]),
        group,
        scatter_dimension=0,
        tiled=True,
    )
    stream = (own_entry.astype(jnp.float32) + mix_total.astype(jnp.float32)).astype(jnp.bfloat16)
    stream_all = lax.all_gather(stream, group, axis=0, tiled=True)
    ffn_normed = normalize(stream_all.astype(jnp.float32), feedforward_norm_factor).astype(
        jnp.bfloat16
    )
    plain = jnp.dot(ffn_normed, ffn_weights[:, : 2 * hidden], preferred_element_type=jnp.float32)
    active = (
        jax.nn.silu(plain[:, :hidden] * part(switch_factors, hidden, 0))
        * (plain[:, hidden:] * part(expand_factors, hidden, 0))
    ).astype(jnp.bfloat16)
    ffn_terms = projected(active, ffn_weights[:, 2 * hidden :], out_scales[1])
    ffn_terms = ffn_terms.reshape(rep, steps, tp, own_features).transpose(0, 2, 1, 3)
    ffn_total = lax.psum_scatter(
        ffn_terms.reshape(rep * tp * steps, own_features), group, scatter_dimension=0, tiled=True
    )
    own_stream = lax.dynamic_slice(
        stream_all, (rep_index * steps, tp_index * own_features), (steps, own_features)
    )
    return (own_stream.astype(jnp.float32) + ffn_total.astype(jnp.float32)).astype(jnp.bfloat16)


MESH = pl.DeviceIdType.MESH
F32 = jnp.float32
BF16 = jnp.bfloat16
RIGHT = (((1,), (0,)), ((), ()))


def dot(a, b):
    return lax.dot_general(a, b, RIGHT, preferred_element_type=F32)


def layer_kernel(
    x_ref,
    wm_ref,
    wb_ref,
    wg_ref,
    wc_ref,
    sc_ref,
    gain_ref,
    ffn_gain_ref,
    mixer_scale_ref,
    rescale_ref,
    ffn_scale_ref,
    place_ref,
    bias_ref,
    out_ref,
    wm_in,
    wb_in,
    wg_in,
    wc_in,
    sc_in,
    x_in,
    xn,
    carrier,
    spread,
    gated,
    sums,
    sums_in,
    parts,
    core_in,
    pair_out,
    pair_in,
    stream,
    active,
    ffn_parts,
    ffn_core_in,
    ffn_pair_out,
    ffn_pair_in,
    send_w,
    recv_w,
    send_sc,
    recv_sc,
    send_a,
    recv_a,
    mixer_channels,
    all_channels,
):
    r = lax.axis_index("rep")
    f = lax.axis_index("fs")
    k = lax.axis_index("tp")
    fx, fy = f % 2, f // 2
    seat = (f, fy * 2 + 1 - fx, (1 - fy) * 2 + fx, 3 - f)
    to_x, to_y, to_d = {"fs": seat[1]}, {"fs": seat[2]}, {"fs": seat[3]}
    to_pair = {"rep": r + 1 - 2 * (r % 2)}
    to_core = {"tp": 1 - k}
    steps = x_ref.shape[0]
    tokens = 2 * steps
    width = wm_ref.shape[0]

    barrier = pltpu.get_barrier_semaphore()
    for other in (to_x, to_y, to_d, to_pair, to_core):
        pl.semaphore_signal(barrier, inc=1, device_id=other, device_id_type=MESH)
    pl.semaphore_wait(barrier, 5)

    def remote(src, dst, send, recv, device):
        return pltpu.make_async_remote_copy(
            src_ref=src, dst_ref=dst, send_sem=send, recv_sem=recv,
            device_id=device, device_id_type=MESH,
        )

    pieces = []
    for ref, buf, n in ((wm_ref, wm_in, 2), (wb_ref, wb_in, 1), (wg_ref, wg_in, 4), (wc_ref, wc_in, 2)):
        size = ref.shape[0] // n
        for i in range(n):
            pieces.append((ref, buf, i * size, size))

    def own(i):
        ref, buf, start, size = pieces[i]
        rows = pl.ds(start, size)
        return (
            remote(ref.at[rows], buf.at[0, rows], send_w.at[i, 0], recv_w.at[i, 0], to_x),
            remote(ref.at[rows], buf.at[1, rows], send_w.at[i, 1], recv_w.at[i, 1], to_y),
        )

    def onward(i):
        ref, buf, start, size = pieces[i]
        first, last = pl.ds(start, size // 2), pl.ds(start + size // 2, size // 2)
        return (
            remote(buf.at[0, first], buf.at[2, first], send_w.at[i, 2], recv_w.at[i, 2], to_y),
            remote(buf.at[1, last], buf.at[2, last], send_w.at[i, 3], recv_w.at[i, 3], to_x),
        )

    def issue(i):
        if i < len(pieces):
            for copy in own(i):
                copy.start()

    def step(i, ahead):
        for copy in own(i):
            copy.wait_recv()
        for copy in onward(i):
            copy.start()
        issue(i + ahead)

    def far(i):
        for copy in onward(i):
            copy.wait_recv()

    scale_copies = [
        remote(sc_ref, sc_in.at[s], send_sc.at[s], recv_sc.at[s], device)
        for s, device in enumerate((to_x, to_y, to_d))
    ]
    x_copy = remote(x_ref, x_in, send_a.at[0], recv_a.at[0], to_pair)
    for copy in scale_copies:
        copy.start()
    issue(0)
    x_copy.start()
    issue(1)

    def feature(s):
        return pl.ds(pl.multiple_of(seat[s] * width, width), width)

    def norm_tile(load, gain, row, size):
        values = [load(s, row).astype(F32) for s in range(4)]
        total = sum(jnp.sum(v * v, axis=1, keepdims=True) for v in values)
        inverse = lax.rsqrt(total / (4 * width) + epsilon)
        for s in range(4):
            xn[s, pl.ds(row, size), :] = (values[s] * inverse * gain[:, feature(s)]).astype(BF16)

    tile = 64

    def norm_own(i, carry):
        norm_tile(lambda s, row: x_ref[pl.ds(row, tile), feature(s)], gain_ref, i * tile, tile)
        return carry

    lax.fori_loop(0, steps // tile, norm_own, 0)
    step(0, 2)
    step(1, 2)
    x_copy.wait_recv()

    def norm_pair(i, carry):
        norm_tile(
            lambda s, row: x_in[pl.ds(i * tile, tile), feature(s)],
            gain_ref, steps + i * tile, tile,
        )
        return carry

    lax.fori_loop(0, steps // tile, norm_pair, 0)
    far(0)
    far(1)

    half = 256
    mixer_in = (wm_ref, wm_in.at[0], wm_in.at[1], wm_in.at[2])

    def mixer_rows(i, carry):
        rows = pl.ds(pl.multiple_of(i * half, half), half)
        plain = dot(xn[0, rows, :], mixer_in[0][...])
        for s in range(1, 4):
            plain += dot(xn[s, rows, :], mixer_in[s][...])
        both = jax.nn.gelu(plain * mixer_scale_ref[...])
        carrier[rows, :] = both[:, :mixer_channels]
        own_spread = both[:, mixer_channels:]
        spread[rows, :] = own_spread
        total = jnp.sum(own_spread * own_spread, axis=1, keepdims=True)
        sums[0, :, rows] = jnp.broadcast_to(total, (half, 128)).T[:8]
        return carry

    lax.fori_loop(0, tokens // half, mixer_rows, 0)
    core_sums = remote(sums.at[0], sums_in.at[0], send_a.at[1], recv_a.at[1], to_core)
    core_sums.start()
    core_sums.wait_recv()
    sums[1] = sums[0] + sums_in[0]
    pair_sums = remote(sums.at[1], sums_in.at[1], send_a.at[2], recv_a.at[2], to_pair)
    pair_sums.start()
    step(2, 2)
    pair_sums.wait_recv()
    received = sums_in[1]
    received = jnp.concatenate((received[:, steps:], received[:, :steps]), axis=1)
    sums[2] = lax.rsqrt((sums[1] + received) / all_channels + epsilon)

    def mix_rows(i, carry):
        rows = pl.ds(pl.multiple_of(i * BLOCK, BLOCK), BLOCK)
        factor = jnp.concatenate([sums[2, :, rows]] * (128 // 8), axis=0).T[:, :1]
        normed = (spread[rows, :] * factor * rescale_ref[...]).astype(BF16)
        for g in range(mixer_channels // GROUP_DIM):
            lanes = pl.ds(g * GROUP_DIM, GROUP_DIM)
            mixed = dot(place_ref[g], normed[:, g * GROUP_DIM : (g + 1) * GROUP_DIM])
            mixed = mixed + bias_ref[:, lanes]
            gated[rows, lanes] = (carrier[rows, lanes] * mixed).astype(BF16)
        return carry

    lax.fori_loop(0, tokens // BLOCK, mix_rows, 0)
    for copy in scale_copies:
        copy.wait_recv()
    scales = (sc_ref, sc_in.at[0], sc_in.at[1], sc_in.at[2])
    keep = (k + fy) % 2
    base = 2 * keep

    def project(values, weights, row, s, target):
        def rows_of(i, carry):
            rows = pl.ds(pl.multiple_of(i * half, half), half)
            target[s, rows, :] = (
                dot(values[rows, :], weights[...]) * scales[s][row : row + 1, :]
            ).astype(BF16)
            return carry

        lax.fori_loop(0, tokens // half, rows_of, 0)

    mixer_out = (wb_ref, wb_in.at[0], wb_in.at[1], wb_in.at[2])
    ffn_out = (wc_ref, wc_in.at[0], wc_in.at[1], wc_in.at[2])

    give = pl.ds(2 - base, 2)
    mix_give = remote(parts.at[give], core_in, send_a.at[3], recv_a.at[3], to_core)
    mix_pair = [
        remote(pair_out.at[j], pair_in.at[j], send_a.at[4 + j], recv_a.at[4 + j], to_pair)
        for j in range(2)
    ]

    def merge_mix():
        mix_give.wait_recv()
        for j in range(2):
            def rows_of(i, carry):
                rows = pl.ds(pl.multiple_of(i * half, half), half)
                pair_out[j, rows, :] = (
                    parts[base + j, rows, :].astype(F32) + core_in[j, rows, :].astype(F32)
                ).astype(BF16)
                return carry

            lax.fori_loop(0, tokens // half, rows_of, 0)
            mix_pair[j].start()

    for t in range(2):
        if t == 1:
            far(2)
        for s in (2 * t, 2 * t + 1):
            project(gated, mixer_out[s], 0, s, parts)

        @pl.when(keep != t)
        def _():
            mix_give.start()

        @pl.when(keep == t)
        def _():
            merge_mix()

    step(3, 2)
    step(4, 2)

    stream_give = [
        remote(stream.at[base + j], stream.at[base + j], send_a.at[6 + j], recv_a.at[6 + j], to_core)
        for j in range(2)
    ]
    stream_take = [
        remote(stream.at[2 - base + j], stream.at[2 - base + j], send_a.at[6 + j], recv_a.at[6 + j], to_core)
        for j in range(2)
    ]
    block_of = (seat[0] + keep * (seat[2] - seat[0]), seat[1] + keep * (seat[3] - seat[1]))
    for j in range(2):
        mix_pair[j].wait_recv()
        lanes = pl.ds(pl.multiple_of(block_of[j] * width, width), width)
        for first, second, source in ((0, steps, x_ref), (steps, 0, x_in)):
            rows = pl.ds(first, steps)
            stream[base + j, rows, :] = (
                source[:, lanes].astype(F32)
                + (
                    pair_out[j, rows, :].astype(F32)
                    + pair_in[j, pl.ds(second, steps), :].astype(F32)
                )
            ).astype(BF16)
        stream_give[j].start()
    for copy in stream_take:
        copy.wait_recv()

    def norm_stream(i, carry):
        norm_tile(
            lambda s, row: stream[s, pl.ds(row, tile), :], ffn_gain_ref, i * tile, tile
        )
        return carry

    lax.fori_loop(0, tokens // tile, norm_stream, 0)
    step(5, 2)
    step(6, 2)
    for i in range(3, 7):
        far(i)

    hidden = active.shape[1]
    ffn_in = (wg_ref, wg_in.at[0], wg_in.at[1], wg_in.at[2])

    def ffn_rows(i, carry):
        rows = pl.ds(pl.multiple_of(i * half, half), half)
        plain = dot(xn[0, rows, :], ffn_in[0][...])
        for s in range(1, 4):
            plain += dot(xn[s, rows, :], ffn_in[s][...])
        plain = plain * ffn_scale_ref[...]
        active[rows, :] = (jax.nn.silu(plain[:, :hidden]) * plain[:, hidden:]).astype(BF16)
        return carry

    lax.fori_loop(0, tokens // half, ffn_rows, 0)
    step(7, 2)
    step(8, 2)

    ffn_give = remote(ffn_parts.at[give], ffn_core_in, send_a.at[8], recv_a.at[8], to_core)
    ffn_pair = [
        remote(ffn_pair_out.at[j], ffn_pair_in.at[j], send_a.at[9 + j], recv_a.at[9 + j], to_pair)
        for j in range(2)
    ]

    def merge_ffn():
        ffn_give.wait_recv()
        rows = pl.ds(steps, steps)
        for j in range(2):
            ffn_pair_out[j] = (
                ffn_parts[base + j, rows, :].astype(F32) + ffn_core_in[j, rows, :].astype(F32)
            ).astype(BF16)
            ffn_pair[j].start()

    for t in range(2):
        if t == 1:
            far(7)
            far(8)
        for s in (2 * t, 2 * t + 1):
            project(active, ffn_out[s], 1, s, ffn_parts)

        @pl.when(keep != t)
        def _():
            ffn_give.start()

        @pl.when(keep == t)
        def _():
            merge_ffn()

    own_rows = pl.ds(0, steps)
    for j in range(2):
        ffn_pair[j].wait_recv()
        column = fx + j - 2 * fx * j
        lanes = pl.ds(pl.multiple_of(column * width, width), width)
        out_ref[:, lanes] = (
            stream[base + j, own_rows, :].astype(F32)
            + (
                ffn_parts[base + j, own_rows, :].astype(F32)
                + ffn_core_in[j, own_rows, :].astype(F32)
                + ffn_pair_in[j].astype(F32)
            )
        ).astype(BF16)

    for i in range(len(pieces)):
        for copy in own(i) + onward(i):
            copy.wait_send()
    for copy in scale_copies + [x_copy, core_sums, pair_sums, mix_give, ffn_give]:
        copy.wait_send()
    for copy in mix_pair + stream_give + ffn_pair:
        copy.wait_send()


def in_one_kernel(

    skip_stream_entry,
    sequence_blender_factor,
    product_projector,
    product_side_factors,
    placewise_projector,
    placewise_entry_factors,
    placewise_rescale_factor,
    place_cluster_operator,
    placewise_offset_vector,
    blender_result_projector,
    blender_result_factors,
    feedforward_norm_factor,
    switch_projector,
    switch_factors,
    expand_projector,
    expand_factors,
    contract_projector,
    contract_factors,
):
    rep_index = lax.axis_index("rep")
    tp_index = lax.axis_index("tp")
    pair_index = rep_index % 2
    steps, embed = skip_stream_entry.shape
    tokens = 2 * steps
    width = product_projector.shape[0]
    channels = product_projector.shape[1] // 2
    hidden = switch_projector.shape[1] // 2
    groups = channels // GROUP_DIM

    def part(values, size, dim):
        return lax.dynamic_slice_in_dim(values, pair_index * size, size, dim)

    def beside(first, second, size):
        return jnp.concatenate(
            (part(first, size, 1).astype(BF16), part(second, size, 1).astype(BF16)), axis=1
        )

    def scales(first, second, size):
        return jnp.concatenate((part(first, size, 0), part(second, size, 0)))[None]

    first_group = (tp_index * 2 + pair_index) * groups
    causal = jnp.tril(jnp.ones((BLOCK, BLOCK), dtype=bool))
    place = lax.dynamic_slice_in_dim(place_cluster_operator, first_group, groups, 0)
    place = jnp.where(causal[None], place, jnp.zeros_like(place))
    bias = lax.dynamic_slice_in_dim(placewise_offset_vector, first_group, groups, 0)
    bias = jnp.repeat(bias.T, GROUP_DIM, axis=1)
    out_scales = jnp.stack((blender_result_factors, contract_factors))
    out_scales = jnp.concatenate((out_scales, jnp.zeros((6, width), F32)))

    vmem = pltpu.VMEM
    dma = pltpu.SemaphoreType.DMA
    blocks = (4, tokens, width)
    two = (2, tokens, width)
    return pl.pallas_call(
        functools.partial(
            layer_kernel,
            mixer_channels=channels,
            all_channels=2 * channels * lax.axis_size("tp"),
        ),
        out_shape=jax.ShapeDtypeStruct((steps, embed // 2), BF16),
        in_specs=[pl.BlockSpec(memory_space=vmem)] * 13,
        out_specs=pl.BlockSpec(memory_space=vmem),
        scratch_shapes=[
            vmem((3, width, 2 * channels), BF16),
            vmem((3, channels, width), BF16),
            vmem((3, width, 2 * hidden), BF16),
            vmem((3, hidden, width), BF16),
            vmem((3, 8, width), F32),
            vmem((steps, embed), BF16),
            vmem(blocks, BF16),
            vmem((tokens, channels), F32),
            vmem((tokens, channels), F32),
            vmem((tokens, channels), BF16),
            vmem((3, 8, tokens), F32),
            vmem((2, 8, tokens), F32),
            vmem(blocks, BF16),
            vmem(two, BF16),
            vmem(two, BF16),
            vmem(two, BF16),
            vmem(blocks, BF16),
            vmem((tokens, hidden), BF16),
            vmem(blocks, BF16),
            vmem(two, BF16),
            vmem((2, steps, width), BF16),
            vmem((2, steps, width), BF16),
            dma((9, 4)),
            dma((9, 4)),
            dma((3,)),
            dma((3,)),
            dma((11,)),
            dma((11,)),
        ],
        compiler_params=pltpu.CompilerParams(
            collective_id=0, has_side_effects=True, vmem_limit_bytes=60 * 1024 * 1024
        ),
    )(
        skip_stream_entry,
        beside(product_projector, placewise_projector, channels),
        part(blender_result_projector, channels, 0).astype(BF16),
        beside(switch_projector, expand_projector, hidden),
        part(contract_projector, hidden, 0).astype(BF16),
        out_scales,
        sequence_blender_factor[None],
        feedforward_norm_factor[None],
        scales(product_side_factors, placewise_entry_factors, channels),
        part(placewise_rescale_factor, channels, 0)[None],
        scales(switch_factors, expand_factors, hidden),
        place,
        bias,
    )


def on_device(*arrays):
    entry, mixer, switch = arrays[0], arrays[2], arrays[12]
    fits = (
        lax.axis_size("rep") % 2 == 0
        and lax.axis_size("fs") == 4
        and lax.axis_size("tp") == 2
        and entry.shape[0] % 256 == 0
        and mixer.shape[0] % 128 == 0
        and mixer.shape[1] % (2 * GROUP_DIM) == 0
        and switch.shape[1] % 128 == 0
    )
    return in_one_kernel(*arrays) if fits else with_collectives(*arrays)


def solution(mesh):
    return jax.shard_map(
        on_device,
        mesh=mesh,
        in_specs=(
            P(("rep", "fs"), None),
            P(),
            P("fs", "tp"),
            P("tp"),
            P("fs", "tp"),
            P("tp"),
            P("tp"),
            P(),
            P(),
            P("tp", "fs"),
            P("fs"),
            P(),
            P("fs", "tp"),
            P("tp"),
            P("fs", "tp"),
            P("tp"),
            P("tp", "fs"),
            P("fs"),
        ),
        out_specs=P(("rep", "fs"), "tp"),
        check_vma=False,
    )
```

```python
import functools

import jax
import jax.numpy as jnp
from jax import lax
from jax.experimental import pallas as pl
from jax.experimental.pallas import tpu as pltpu
from jax.sharding import PartitionSpec as P

BLENDER_FEATURES = 1024
GROUP_DIM = 128
BLOCK = 128


epsilon = 1e-06


def normalize(values, gain):
    return values * lax.rsqrt(jnp.mean(values * values, axis=-1, keepdims=True) + epsilon) * gain


def with_collectives(
    skip_stream_entry,
    sequence_blender_factor,
    product_projector,
    product_side_factors,
    placewise_projector,
    placewise_entry_factors,
    placewise_rescale_factor,
    place_cluster_operator,
    placewise_offset_vector,
    blender_result_projector,
    blender_result_factors,
    feedforward_norm_factor,
    switch_projector,
    switch_factors,
    expand_projector,
    expand_factors,
    contract_projector,
    contract_factors,
):
    rep = lax.axis_size("rep")
    tp = lax.axis_size("tp")
    rep_index = lax.axis_index("rep")
    tp_index = lax.axis_index("tp")
    group = ("rep", "tp")
    steps, embed = skip_stream_entry.shape
    own_steps = steps // tp
    own_features = embed // tp
    channels = product_projector.shape[1] // rep
    hidden = switch_projector.shape[1] // rep

    def part(values, size, dim):
        return lax.dynamic_slice_in_dim(values, rep_index * size, size, dim)

    def gathered(first, second, out, size):
        return lax.all_gather(
            jnp.concatenate(
                (
                    part(first, size, 1).astype(jnp.bfloat16),
                    part(second, size, 1).astype(jnp.bfloat16),
                    part(out, size, 0).astype(jnp.bfloat16).T,
                ),
                axis=1,
            ),
            "fs",
            axis=0,
            tiled=True,
        )

    own_entry = lax.dynamic_slice_in_dim(skip_stream_entry, tp_index * own_steps, own_steps, 0)
    normed = lax.all_gather(
        normalize(own_entry.astype(jnp.float32), sequence_blender_factor).astype(jnp.bfloat16),
        group,
        axis=0,
        tiled=True,
    )
    mixer_weights = gathered(
        product_projector, placewise_projector, blender_result_projector, channels
    )
    out_scales = lax.all_gather(
        jnp.stack((blender_result_factors, contract_factors)), "fs", axis=1, tiled=True
    )
    ffn_weights = gathered(switch_projector, expand_projector, contract_projector, hidden)

    tokens = normed.shape[0]
    plain = jnp.dot(normed, mixer_weights[:, : 2 * channels], preferred_element_type=jnp.float32)
    carrier = jax.nn.gelu(plain[:, :channels] * part(product_side_factors, channels, 0))
    spread = jax.nn.gelu(plain[:, channels:] * part(placewise_entry_factors, channels, 0))
    squares = lax.psum(jnp.sum(spread * spread, axis=1), group)
    factor = lax.rsqrt(squares / BLENDER_FEATURES + epsilon)
    spread_normed = (
        spread * factor[:, None] * part(placewise_rescale_factor, channels, 0)
    ).astype(jnp.bfloat16)
    span = min(channels, GROUP_DIM)
    count = max(1, channels // GROUP_DIM)
    first_group = (tp_index * rep + rep_index) * channels // GROUP_DIM
    causal = jnp.tril(jnp.ones((BLOCK, BLOCK), dtype=bool))
    local_weight = lax.dynamic_slice_in_dim(place_cluster_operator, first_group, count, 0)
    local_weight = jnp.where(causal[None], local_weight, jnp.zeros_like(local_weight))
    local_bias = lax.dynamic_slice_in_dim(placewise_offset_vector, first_group, count, 0)
    blocks = spread_normed.reshape(tokens // BLOCK, BLOCK, count, span)
    mixed = jnp.einsum("gts,nsgc->ntgc", local_weight, blocks, preferred_element_type=jnp.float32)
    mixed = mixed + local_bias.T[None, :, :, None]
    gated = (carrier * mixed.reshape(tokens, channels)).astype(jnp.bfloat16)

    def projected(values, weights, scales):
        return (
            lax.dot_general(
                values, weights, (((1,), (1,)), ((), ())), preferred_element_type=jnp.float32
            )
            * scales
        ).astype(jnp.bfloat16)

    mix_total = lax.psum_scatter(
        projected(gated, mixer_weights[:, 2 * channels :], out_scales[0]),
        group,
        scatter_dimension=0,
        tiled=True,
    )
    stream = (own_entry.astype(jnp.float32) + mix_total.astype(jnp.float32)).astype(jnp.bfloat16)
    stream_all = lax.all_gather(stream, group, axis=0, tiled=True)
    ffn_normed = normalize(stream_all.astype(jnp.float32), feedforward_norm_factor).astype(
        jnp.bfloat16
    )
    plain = jnp.dot(ffn_normed, ffn_weights[:, : 2 * hidden], preferred_element_type=jnp.float32)
    active = (
        jax.nn.silu(plain[:, :hidden] * part(switch_factors, hidden, 0))
        * (plain[:, hidden:] * part(expand_factors, hidden, 0))
    ).astype(jnp.bfloat16)
    ffn_terms = projected(active, ffn_weights[:, 2 * hidden :], out_scales[1])
    ffn_terms = ffn_terms.reshape(rep, steps, tp, own_features).transpose(0, 2, 1, 3)
    ffn_total = lax.psum_scatter(
        ffn_terms.reshape(rep * tp * steps, own_features), group, scatter_dimension=0, tiled=True
    )
    own_stream = lax.dynamic_slice(
        stream_all, (rep_index * steps, tp_index * own_features), (steps, own_features)
    )
    return (own_stream.astype(jnp.float32) + ffn_total.astype(jnp.float32)).astype(jnp.bfloat16)


MESH = pl.DeviceIdType.MESH
F32 = jnp.float32
BF16 = jnp.bfloat16
RIGHT = (((1,), (0,)), ((), ()))


def dot(a, b):
    return lax.dot_general(a, b, RIGHT, preferred_element_type=F32)


def layer_kernel(
    x_ref,
    product_ref,
    placewise_ref,
    blender_ref,
    switch_ref,
    expand_ref,
    contract_ref,
    gain_ref,
    ffn_gain_ref,
    product_scale_ref,
    placewise_scale_ref,
    rescale_ref,
    switch_scale_ref,
    expand_scale_ref,
    mix_scale_ref,
    contract_scale_ref,
    place_ref,
    bias_ref,
    out_ref,
    wm_ref,
    wb_ref,
    wg_ref,
    wc_ref,
    sc_ref,
    wm_wide,
    wb_wide,
    wg_wide,
    wc_wide,
    wm_in,
    wb_in,
    wg_in,
    wc_in,
    sc_in,
    x_in,
    xn,
    carrier,
    spread,
    gated,
    sums,
    sums_in,
    parts,
    core_in,
    pair_out,
    pair_in,
    stream,
    active,
    ffn_parts,
    ffn_core_in,
    ffn_pair_out,
    ffn_pair_in,
    send_w,
    recv_w,
    send_sc,
    recv_sc,
    send_a,
    recv_a,
    load,
    mixer_channels,
    all_channels,
):
    r = lax.axis_index("rep")
    f = lax.axis_index("fs")
    k = lax.axis_index("tp")
    fx, fy = f % 2, f // 2
    seat = (f, fy * 2 + 1 - fx, (1 - fy) * 2 + fx, 3 - f)
    to_x, to_y, to_d = {"fs": seat[1]}, {"fs": seat[2]}, {"fs": seat[3]}
    to_pair = {"rep": r + 1 - 2 * (r % 2)}
    to_core = {"tp": 1 - k}
    steps = x_ref.shape[0]
    tokens = 2 * steps
    width = wm_ref.shape[0]
    h = r % 2
    hidden = active.shape[1]
    shard = pl.ds(pl.multiple_of(h * mixer_channels, mixer_channels), mixer_channels)
    units = pl.ds(pl.multiple_of(h * hidden, 8), hidden)
    loads = [
        pltpu.make_async_copy(src, dst, load.at[i])
        for i, (src, dst) in enumerate(
            (
                (product_ref.at[:, shard], wm_wide.at[0]),
                (placewise_ref.at[:, shard], wm_wide.at[1]),
                (blender_ref.at[shard], wb_wide),
                (switch_ref, wg_wide.at[0]),
                (expand_ref, wg_wide.at[1]),
                (contract_ref.at[units], wc_wide),
            )
        )
    ]
    for copy in loads:
        copy.start()

    def chosen(values):
        return jnp.where(h == 0, values[:, :hidden], values[:, hidden:])

    first_row = lax.broadcasted_iota(jnp.int32, sc_ref.shape, 0) == 0
    sc_ref[...] = jnp.where(first_row, mix_scale_ref[...], contract_scale_ref[...])

    barrier = pltpu.get_barrier_semaphore()
    for other in (to_x, to_y, to_d, to_pair, to_core):
        pl.semaphore_signal(barrier, inc=1, device_id=other, device_id_type=MESH)
    pl.semaphore_wait(barrier, 5)

    def remote(src, dst, send, recv, device):
        return pltpu.make_async_remote_copy(
            src_ref=src, dst_ref=dst, send_sem=send, recv_sem=recv,
            device_id=device, device_id_type=MESH,
        )

    pieces = []
    for ref, buf, n in ((wm_ref, wm_in, 2), (wb_ref, wb_in, 1), (wg_ref, wg_in, 4), (wc_ref, wc_in, 2)):
        size = ref.shape[0] // n
        for i in range(n):
            pieces.append((ref, buf, i * size, size))

    def own(i):
        ref, buf, start, size = pieces[i]
        rows = pl.ds(start, size)
        return (
            remote(ref.at[rows], buf.at[0, rows], send_w.at[i, 0], recv_w.at[i, 0], to_x),
            remote(ref.at[rows], buf.at[1, rows], send_w.at[i, 1], recv_w.at[i, 1], to_y),
        )

    def onward(i):
        ref, buf, start, size = pieces[i]
        first, last = pl.ds(start, size // 2), pl.ds(start + size // 2, size // 2)
        return (
            remote(buf.at[0, first], buf.at[2, first], send_w.at[i, 2], recv_w.at[i, 2], to_y),
            remote(buf.at[1, last], buf.at[2, last], send_w.at[i, 3], recv_w.at[i, 3], to_x),
        )

    def issue(i):
        if i < len(pieces):
            for copy in own(i):
                copy.start()

    def step(i, ahead):
        for copy in own(i):
            copy.wait_recv()
        for copy in onward(i):
            copy.start()
        issue(i + ahead)

    def far(i):
        for copy in onward(i):
            copy.wait_recv()

    scale_copies = [
        remote(sc_ref, sc_in.at[s], send_sc.at[s], recv_sc.at[s], device)
        for s, device in enumerate((to_x, to_y, to_d))
    ]
    x_copy = remote(x_ref, x_in, send_a.at[0], recv_a.at[0], to_pair)
    loads[0].wait()
    loads[1].wait()
    wm_ref[:, :mixer_channels] = wm_wide[0].astype(BF16)
    wm_ref[:, mixer_channels:] = wm_wide[1].astype(BF16)
    x_copy.start()
    for copy in scale_copies:
        copy.start()
    issue(0)
    issue(1)
    loads[2].wait()
    wb_ref[...] = wb_wide[...].astype(BF16)
    loads[3].wait()
    loads[4].wait()

    def round_ffn(i, carry):
        rows = pl.ds(pl.multiple_of(i * 64, 64), 64)
        wg_ref[rows, :] = jnp.concatenate(
            (chosen(wg_wide[0, rows, :]), chosen(wg_wide[1, rows, :])), axis=1
        ).astype(BF16)
        return carry

    lax.fori_loop(0, width // 64, round_ffn, 0)
    loads[5].wait()
    wc_ref[...] = wc_wide[...].astype(BF16)

    def feature(s):
        return pl.ds(pl.multiple_of(seat[s] * width, width), width)

    def norm_tile(load, gain, row, size):
        values = [load(s, row).astype(F32) for s in range(4)]
        total = sum(jnp.sum(v * v, axis=1, keepdims=True) for v in values)
        inverse = lax.rsqrt(total / (4 * width) + epsilon)
        for s in range(4):
            xn[s, pl.ds(row, size), :] = (values[s] * inverse * gain[:, feature(s)]).astype(BF16)

    tile = 64

    def norm_own(i, carry):
        norm_tile(lambda s, row: x_ref[pl.ds(row, tile), feature(s)], gain_ref, i * tile, tile)
        return carry

    lax.fori_loop(0, steps // tile, norm_own, 0)
    step(0, 2)
    step(1, 2)
    x_copy.wait_recv()

    def norm_pair(i, carry):
        norm_tile(
            lambda s, row: x_in[pl.ds(i * tile, tile), feature(s)],
            gain_ref, steps + i * tile, tile,
        )
        return carry

    lax.fori_loop(0, steps // tile, norm_pair, 0)
    far(0)
    far(1)

    half = 256
    mixer_in = (wm_ref, wm_in.at[0], wm_in.at[1], wm_in.at[2])

    def mixer_rows(i, carry):
        rows = pl.ds(pl.multiple_of(i * half, half), half)
        plain = dot(xn[0, rows, :], mixer_in[0][...])
        for s in range(1, 4):
            plain += dot(xn[s, rows, :], mixer_in[s][...])
        column_scales = jnp.concatenate(
            (product_scale_ref[:, shard], placewise_scale_ref[:, shard]), axis=1
        )
        both = jax.nn.gelu(plain * column_scales)
        carrier[rows, :] = both[:, :mixer_channels]
        own_spread = both[:, mixer_channels:]
        spread[rows, :] = own_spread
        total = jnp.sum(own_spread * own_spread, axis=1, keepdims=True)
        sums[0, :, rows] = jnp.broadcast_to(total, (half, 128)).T[:8]
        return carry

    lax.fori_loop(0, tokens // half, mixer_rows, 0)
    core_sums = remote(sums.at[0], sums_in.at[0], send_a.at[1], recv_a.at[1], to_core)
    core_sums.start()
    core_sums.wait_recv()
    sums[1] = sums[0] + sums_in[0]
    pair_sums = remote(sums.at[1], sums_in.at[1], send_a.at[2], recv_a.at[2], to_pair)
    pair_sums.start()
    step(2, 2)
    issue(5)
    pair_sums.wait_recv()
    received = sums_in[1]
    received = jnp.concatenate((received[:, steps:], received[:, :steps]), axis=1)
    sums[2] = lax.rsqrt((sums[1] + received) / all_channels + epsilon)

    causal = lax.broadcasted_iota(jnp.int32, (BLOCK, BLOCK), 0) >= lax.broadcasted_iota(
        jnp.int32, (BLOCK, BLOCK), 1
    )
    groups = mixer_channels // GROUP_DIM
    first_group = (2 * k + h) * groups

    def mix_rows(i, carry):
        rows = pl.ds(pl.multiple_of(i * BLOCK, BLOCK), BLOCK)
        factor = jnp.concatenate([sums[2, :, rows]] * (128 // 8), axis=0).T[:, :1]
        normed = (spread[rows, :] * factor * rescale_ref[:, shard]).astype(BF16)
        for g in range(groups):
            lanes = pl.ds(g * GROUP_DIM, GROUP_DIM)
            operator = place_ref[first_group + g]
            operator = jnp.where(causal, operator, jnp.zeros_like(operator))
            offset = jnp.broadcast_to(bias_ref[pl.ds(first_group + g, 1), :], (BLOCK, BLOCK)).T
            mixed = dot(operator, normed[:, g * GROUP_DIM : (g + 1) * GROUP_DIM])
            mixed = mixed + offset
            gated[rows, lanes] = (carrier[rows, lanes] * mixed).astype(BF16)
        return carry

    lax.fori_loop(0, tokens // BLOCK, mix_rows, 0)
    for copy in scale_copies:
        copy.wait_recv()
    scales = (sc_ref, sc_in.at[0], sc_in.at[1], sc_in.at[2])
    keep = (k + fy) % 2
    base = 2 * keep

    def project(values, weights, row, s, target):
        def rows_of(i, carry):
            rows = pl.ds(pl.multiple_of(i * half, half), half)
            target[s, rows, :] = (
                dot(values[rows, :], weights[...]) * scales[s][row : row + 1, :]
            ).astype(BF16)
            return carry

        lax.fori_loop(0, tokens // half, rows_of, 0)

    mixer_out = (wb_ref, wb_in.at[0], wb_in.at[1], wb_in.at[2])
    ffn_out = (wc_ref, wc_in.at[0], wc_in.at[1], wc_in.at[2])

    give = pl.ds(2 - base, 2)
    mix_give = remote(parts.at[give], core_in, send_a.at[3], recv_a.at[3], to_core)
    mix_pair = [
        remote(pair_out.at[j], pair_in.at[j], send_a.at[4 + j], recv_a.at[4 + j], to_pair)
        for j in range(2)
    ]

    def merge_mix():
        mix_give.wait_recv()
        for j in range(2):
            def rows_of(i, carry):
                rows = pl.ds(pl.multiple_of(i * half, half), half)
                pair_out[j, rows, :] = (
                    parts[base + j, rows, :].astype(F32) + core_in[j, rows, :].astype(F32)
                ).astype(BF16)
                return carry

            lax.fori_loop(0, tokens // half, rows_of, 0)
            mix_pair[j].start()

    for t in range(2):
        if t == 1:
            far(2)
        for s in (2 * t, 2 * t + 1):
            project(gated, mixer_out[s], 0, s, parts)

        @pl.when(keep != t)
        def _():
            mix_give.start()

        @pl.when(keep == t)
        def _():
            merge_mix()

    step(3, 3)
    step(4, len(pieces))

    stream_give = [
        remote(stream.at[base + j], stream.at[base + j], send_a.at[6 + j], recv_a.at[6 + j], to_core)
        for j in range(2)
    ]
    stream_take = [
        remote(stream.at[2 - base + j], stream.at[2 - base + j], send_a.at[6 + j], recv_a.at[6 + j], to_core)
        for j in range(2)
    ]
    block_of = (seat[0] + keep * (seat[2] - seat[0]), seat[1] + keep * (seat[3] - seat[1]))
    for j in range(2):
        mix_pair[j].wait_recv()
        lanes = pl.ds(pl.multiple_of(block_of[j] * width, width), width)
        for first, second, source in ((0, steps, x_ref), (steps, 0, x_in)):
            rows = pl.ds(first, steps)
            stream[base + j, rows, :] = (
                source[:, lanes].astype(F32)
                + (
                    pair_out[j, rows, :].astype(F32)
                    + pair_in[j, pl.ds(second, steps), :].astype(F32)
                )
            ).astype(BF16)
        stream_give[j].start()
    for copy in stream_take:
        copy.wait_recv()

    def norm_stream(i, carry):
        norm_tile(
            lambda s, row: stream[s, pl.ds(row, tile), :], ffn_gain_ref, i * tile, tile
        )
        return carry

    lax.fori_loop(0, tokens // tile, norm_stream, 0)
    step(5, 2)
    step(6, 2)
    for i in range(3, 7):
        far(i)

    ffn_in = (wg_ref, wg_in.at[0], wg_in.at[1], wg_in.at[2])

    def ffn_rows(i, carry):
        rows = pl.ds(pl.multiple_of(i * half, half), half)
        plain = dot(xn[0, rows, :], ffn_in[0][...])
        for s in range(1, 4):
            plain += dot(xn[s, rows, :], ffn_in[s][...])
        plain = plain * jnp.concatenate(
            (chosen(switch_scale_ref[...]), chosen(expand_scale_ref[...])), axis=1
        )
        active[rows, :] = (jax.nn.silu(plain[:, :hidden]) * plain[:, hidden:]).astype(BF16)
        return carry

    lax.fori_loop(0, tokens // half, ffn_rows, 0)
    step(7, 2)
    step(8, 2)

    ffn_give = remote(ffn_parts.at[give], ffn_core_in, send_a.at[8], recv_a.at[8], to_core)
    ffn_pair = [
        remote(ffn_pair_out.at[j], ffn_pair_in.at[j], send_a.at[9 + j], recv_a.at[9 + j], to_pair)
        for j in range(2)
    ]

    def merge_ffn():
        ffn_give.wait_recv()
        rows = pl.ds(steps, steps)
        for j in range(2):
            ffn_pair_out[j] = (
                ffn_parts[base + j, rows, :].astype(F32) + ffn_core_in[j, rows, :].astype(F32)
            ).astype(BF16)
            ffn_pair[j].start()

    for t in range(2):
        if t == 1:
            far(7)
            far(8)
        for s in (2 * t, 2 * t + 1):
            project(active, ffn_out[s], 1, s, ffn_parts)

        @pl.when(keep != t)
        def _():
            ffn_give.start()

        @pl.when(keep == t)
        def _():
            merge_ffn()

    own_rows = pl.ds(0, steps)
    for j in range(2):
        ffn_pair[j].wait_recv()
        column = fx + j - 2 * fx * j
        lanes = pl.ds(pl.multiple_of(column * width, width), width)
        out_ref[:, lanes] = (
            stream[base + j, own_rows, :].astype(F32)
            + (
                ffn_parts[base + j, own_rows, :].astype(F32)
                + ffn_core_in[j, own_rows, :].astype(F32)
                + ffn_pair_in[j].astype(F32)
            )
        ).astype(BF16)

    for i in range(len(pieces)):
        for copy in own(i) + onward(i):
            copy.wait_send()
    for copy in scale_copies + [x_copy, core_sums, pair_sums, mix_give, ffn_give]:
        copy.wait_send()
    for copy in mix_pair + stream_give + ffn_pair:
        copy.wait_send()


def in_one_kernel(

    skip_stream_entry,
    sequence_blender_factor,
    product_projector,
    product_side_factors,
    placewise_projector,
    placewise_entry_factors,
    placewise_rescale_factor,
    place_cluster_operator,
    placewise_offset_vector,
    blender_result_projector,
    blender_result_factors,
    feedforward_norm_factor,
    switch_projector,
    switch_factors,
    expand_projector,
    expand_factors,
    contract_projector,
    contract_factors,
):
    steps, embed = skip_stream_entry.shape
    tokens = 2 * steps
    width = product_projector.shape[0]
    channels = product_projector.shape[1] // 2
    hidden = switch_projector.shape[1] // 2

    vmem = pltpu.VMEM
    dma = pltpu.SemaphoreType.DMA
    blocks = (4, tokens, width)
    two = (2, tokens, width)
    return pl.pallas_call(
        functools.partial(
            layer_kernel,
            mixer_channels=channels,
            all_channels=2 * channels * lax.axis_size("tp"),
        ),
        out_shape=jax.ShapeDtypeStruct((steps, embed // 2), BF16),
        in_specs=[pl.BlockSpec(memory_space=vmem)]
        + [pl.BlockSpec(memory_space=pl.ANY)] * 6
        + [pl.BlockSpec(memory_space=vmem)] * 11,
        out_specs=pl.BlockSpec(memory_space=vmem),
        scratch_shapes=[
            vmem((width, 2 * channels), BF16),
            vmem((channels, width), BF16),
            vmem((width, 2 * hidden), BF16),
            vmem((hidden, width), BF16),
            vmem((8, width), F32),
            vmem((2, width, channels), F32),
            vmem((channels, width), F32),
            vmem((2, width, 2 * hidden), F32),
            vmem((hidden, width), F32),
            vmem((3, width, 2 * channels), BF16),
            vmem((3, channels, width), BF16),
            vmem((3, width, 2 * hidden), BF16),
            vmem((3, hidden, width), BF16),
            vmem((3, 8, width), F32),
            vmem((steps, embed), BF16),
            vmem(blocks, BF16),
            vmem((tokens, channels), F32),
            vmem((tokens, channels), F32),
            vmem((tokens, channels), BF16),
            vmem((3, 8, tokens), F32),
            vmem((2, 8, tokens), F32),
            vmem(blocks, BF16),
            vmem(two, BF16),
            vmem(two, BF16),
            vmem(two, BF16),
            vmem(blocks, BF16),
            vmem((tokens, hidden), BF16),
            vmem(blocks, BF16),
            vmem(two, BF16),
            vmem((2, steps, width), BF16),
            vmem((2, steps, width), BF16),
            dma((9, 4)),
            dma((9, 4)),
            dma((3,)),
            dma((3,)),
            dma((11,)),
            dma((11,)),
            dma((6,)),
        ],
        compiler_params=pltpu.CompilerParams(
            collective_id=0, has_side_effects=True, vmem_limit_bytes=60 * 1024 * 1024
        ),
    )(
        skip_stream_entry,
        product_projector,
        placewise_projector,
        blender_result_projector,
        switch_projector,
        expand_projector,
        contract_projector,
        sequence_blender_factor[None],
        feedforward_norm_factor[None],
        product_side_factors[None],
        placewise_entry_factors[None],
        placewise_rescale_factor[None],
        switch_factors[None],
        expand_factors[None],
        blender_result_factors[None],
        contract_factors[None],
        place_cluster_operator,
        placewise_offset_vector,
    )


def on_device(*arrays):
    entry, mixer, switch = arrays[0], arrays[2], arrays[12]
    fits = (
        lax.axis_size("rep") % 2 == 0
        and lax.axis_size("fs") == 4
        and lax.axis_size("tp") == 2
        and entry.shape[0] % 256 == 0
        and mixer.shape[0] % 128 == 0
        and mixer.shape[1] % (2 * GROUP_DIM) == 0
        and switch.shape[1] % 128 == 0
    )
    return in_one_kernel(*arrays) if fits else with_collectives(*arrays)


def solution(mesh):
    return jax.shard_map(
        on_device,
        mesh=mesh,
        in_specs=(
            P(("rep", "fs"), None),
            P(),
            P("fs", "tp"),
            P("tp"),
            P("fs", "tp"),
            P("tp"),
            P("tp"),
            P(),
            P(),
            P("tp", "fs"),
            P("fs"),
            P(),
            P("fs", "tp"),
            P("tp"),
            P("fs", "tp"),
            P("tp"),
            P("tp", "fs"),
            P("fs"),
        ),
        out_specs=P(("rep", "fs"), "tp"),
        check_vma=False,
    )
```

```python
import functools

import jax
import jax.numpy as jnp
from jax import lax
from jax.experimental import pallas as pl
from jax.experimental.pallas import tpu as pltpu
from jax.sharding import PartitionSpec as P

BLENDER_FEATURES = 1024
GROUP_DIM = 128
BLOCK = 128


epsilon = 1e-06


def normalize(values, gain):
    return values * lax.rsqrt(jnp.mean(values * values, axis=-1, keepdims=True) + epsilon) * gain


def with_collectives(
    skip_stream_entry,
    sequence_blender_factor,
    product_projector,
    product_side_factors,
    placewise_projector,
    placewise_entry_factors,
    placewise_rescale_factor,
    place_cluster_operator,
    placewise_offset_vector,
    blender_result_projector,
    blender_result_factors,
    feedforward_norm_factor,
    switch_projector,
    switch_factors,
    expand_projector,
    expand_factors,
    contract_projector,
    contract_factors,
):
    rep = lax.axis_size("rep")
    tp = lax.axis_size("tp")
    rep_index = lax.axis_index("rep")
    tp_index = lax.axis_index("tp")
    group = ("rep", "tp")
    steps, embed = skip_stream_entry.shape
    own_steps = steps // tp
    own_features = embed // tp
    channels = product_projector.shape[1] // rep
    hidden = switch_projector.shape[1] // rep

    def part(values, size, dim):
        return lax.dynamic_slice_in_dim(values, rep_index * size, size, dim)

    def gathered(first, second, out, size):
        return lax.all_gather(
            jnp.concatenate(
                (
                    part(first, size, 1).astype(jnp.bfloat16),
                    part(second, size, 1).astype(jnp.bfloat16),
                    part(out, size, 0).astype(jnp.bfloat16).T,
                ),
                axis=1,
            ),
            "fs",
            axis=0,
            tiled=True,
        )

    own_entry = lax.dynamic_slice_in_dim(skip_stream_entry, tp_index * own_steps, own_steps, 0)
    normed = lax.all_gather(
        normalize(own_entry.astype(jnp.float32), sequence_blender_factor).astype(jnp.bfloat16),
        group,
        axis=0,
        tiled=True,
    )
    mixer_weights = gathered(
        product_projector, placewise_projector, blender_result_projector, channels
    )
    out_scales = lax.all_gather(
        jnp.stack((blender_result_factors, contract_factors)), "fs", axis=1, tiled=True
    )
    ffn_weights = gathered(switch_projector, expand_projector, contract_projector, hidden)

    tokens = normed.shape[0]
    plain = jnp.dot(normed, mixer_weights[:, : 2 * channels], preferred_element_type=jnp.float32)
    carrier = jax.nn.gelu(plain[:, :channels] * part(product_side_factors, channels, 0))
    spread = jax.nn.gelu(plain[:, channels:] * part(placewise_entry_factors, channels, 0))
    squares = lax.psum(jnp.sum(spread * spread, axis=1), group)
    factor = lax.rsqrt(squares / BLENDER_FEATURES + epsilon)
    spread_normed = (
        spread * factor[:, None] * part(placewise_rescale_factor, channels, 0)
    ).astype(jnp.bfloat16)
    span = min(channels, GROUP_DIM)
    count = max(1, channels // GROUP_DIM)
    first_group = (tp_index * rep + rep_index) * channels // GROUP_DIM
    causal = jnp.tril(jnp.ones((BLOCK, BLOCK), dtype=bool))
    local_weight = lax.dynamic_slice_in_dim(place_cluster_operator, first_group, count, 0)
    local_weight = jnp.where(causal[None], local_weight, jnp.zeros_like(local_weight))
    local_bias = lax.dynamic_slice_in_dim(placewise_offset_vector, first_group, count, 0)
    blocks = spread_normed.reshape(tokens // BLOCK, BLOCK, count, span)
    mixed = jnp.einsum("gts,nsgc->ntgc", local_weight, blocks, preferred_element_type=jnp.float32)
    mixed = mixed + local_bias.T[None, :, :, None]
    gated = (carrier * mixed.reshape(tokens, channels)).astype(jnp.bfloat16)

    def projected(values, weights, scales):
        return (
            lax.dot_general(
                values, weights, (((1,), (1,)), ((), ())), preferred_element_type=jnp.float32
            )
            * scales
        ).astype(jnp.bfloat16)

    mix_total = lax.psum_scatter(
        projected(gated, mixer_weights[:, 2 * channels :], out_scales[0]),
        group,
        scatter_dimension=0,
        tiled=True,
    )
    stream = (own_entry.astype(jnp.float32) + mix_total.astype(jnp.float32)).astype(jnp.bfloat16)
    stream_all = lax.all_gather(stream, group, axis=0, tiled=True)
    ffn_normed = normalize(stream_all.astype(jnp.float32), feedforward_norm_factor).astype(
        jnp.bfloat16
    )
    plain = jnp.dot(ffn_normed, ffn_weights[:, : 2 * hidden], preferred_element_type=jnp.float32)
    active = (
        jax.nn.silu(plain[:, :hidden] * part(switch_factors, hidden, 0))
        * (plain[:, hidden:] * part(expand_factors, hidden, 0))
    ).astype(jnp.bfloat16)
    ffn_terms = projected(active, ffn_weights[:, 2 * hidden :], out_scales[1])
    ffn_terms = ffn_terms.reshape(rep, steps, tp, own_features).transpose(0, 2, 1, 3)
    ffn_total = lax.psum_scatter(
        ffn_terms.reshape(rep * tp * steps, own_features), group, scatter_dimension=0, tiled=True
    )
    own_stream = lax.dynamic_slice(
        stream_all, (rep_index * steps, tp_index * own_features), (steps, own_features)
    )
    return (own_stream.astype(jnp.float32) + ffn_total.astype(jnp.float32)).astype(jnp.bfloat16)


MESH = pl.DeviceIdType.MESH
F32 = jnp.float32
BF16 = jnp.bfloat16
RIGHT = (((1,), (0,)), ((), ()))


def dot(a, b):
    return lax.dot_general(a, b, RIGHT, preferred_element_type=F32)


def layer_kernel(
    x_ref,
    product_ref,
    placewise_ref,
    blender_ref,
    switch_ref,
    expand_ref,
    contract_ref,
    gain_ref,
    ffn_gain_ref,
    product_scale_ref,
    placewise_scale_ref,
    rescale_ref,
    switch_scale_ref,
    expand_scale_ref,
    mix_scale_ref,
    contract_scale_ref,
    place_ref,
    bias_ref,
    out_ref,
    wm_ref,
    wb_ref,
    wg_ref,
    wc_ref,
    sc_ref,
    wm_wide,
    wb_wide,
    wg_wide,
    wc_wide,
    wm_in,
    wb_in,
    wg_in,
    wc_in,
    sc_in,
    x_in,
    xn,
    carrier,
    spread,
    gated,
    sums,
    sums_in,
    parts,
    core_in,
    pair_out,
    pair_in,
    stream,
    active,
    ffn_parts,
    ffn_core_in,
    ffn_pair_out,
    ffn_pair_in,
    send_w,
    recv_w,
    send_sc,
    recv_sc,
    send_a,
    recv_a,
    load,
    mixer_channels,
    all_channels,
):
    r = lax.axis_index("rep")
    f = lax.axis_index("fs")
    k = lax.axis_index("tp")
    fx, fy = f % 2, f // 2
    seat = (f, fy * 2 + 1 - fx, (1 - fy) * 2 + fx, 3 - f)
    to_x, to_y, to_d = {"fs": seat[1]}, {"fs": seat[2]}, {"fs": seat[3]}
    to_pair = {"rep": r + 1 - 2 * (r % 2)}
    to_core = {"tp": 1 - k}
    steps = x_ref.shape[0]
    tokens = 2 * steps
    width = wm_ref.shape[0]
    h = r % 2
    hidden = active.shape[1]
    shard = pl.ds(pl.multiple_of(h * mixer_channels, mixer_channels), mixer_channels)
    units = pl.ds(pl.multiple_of(h * hidden, 8), hidden)
    loads = [
        pltpu.make_async_copy(src, dst, load.at[i])
        for i, (src, dst) in enumerate(
            (
                (product_ref.at[:, shard], wm_wide.at[0]),
                (placewise_ref.at[:, shard], wm_wide.at[1]),
                (blender_ref.at[shard], wb_wide),
                (switch_ref, wg_wide.at[0]),
                (expand_ref, wg_wide.at[1]),
                (contract_ref.at[units], wc_wide),
            )
        )
    ]
    for copy in loads:
        copy.start()

    def chosen(values):
        return jnp.where(h == 0, values[:, :hidden], values[:, hidden:])

    first_row = lax.broadcasted_iota(jnp.int32, sc_ref.shape, 0) == 0
    sc_ref[...] = jnp.where(first_row, mix_scale_ref[...], contract_scale_ref[...])

    barrier = pltpu.get_barrier_semaphore()
    for other in (to_x, to_y, to_d, to_pair, to_core):
        pl.semaphore_signal(barrier, inc=1, device_id=other, device_id_type=MESH)
    pl.semaphore_wait(barrier, 5)

    def remote(src, dst, send, recv, device):
        return pltpu.make_async_remote_copy(
            src_ref=src, dst_ref=dst, send_sem=send, recv_sem=recv,
            device_id=device, device_id_type=MESH,
        )

    pieces = []
    for ref, buf, n in ((wm_ref, wm_in, 2), (wb_ref, wb_in, 1), (wg_ref, wg_in, 4), (wc_ref, wc_in, 2)):
        size = ref.shape[0] // n
        for i in range(n):
            pieces.append((ref, buf, i * size, size))

    def own(i):
        ref, buf, start, size = pieces[i]
        rows = pl.ds(start, size)
        return (
            remote(ref.at[rows], buf.at[0, rows], send_w.at[i, 0], recv_w.at[i, 0], to_x),
            remote(ref.at[rows], buf.at[1, rows], send_w.at[i, 1], recv_w.at[i, 1], to_y),
        )

    def onward(i):
        ref, buf, start, size = pieces[i]
        first, last = pl.ds(start, size // 2), pl.ds(start + size // 2, size // 2)
        return (
            remote(buf.at[0, first], buf.at[2, first], send_w.at[i, 2], recv_w.at[i, 2], to_y),
            remote(buf.at[1, last], buf.at[2, last], send_w.at[i, 3], recv_w.at[i, 3], to_x),
        )

    def issue(i):
        if i < len(pieces):
            for copy in own(i):
                copy.start()

    def step(i, ahead):
        for copy in own(i):
            copy.wait_recv()
        for copy in onward(i):
            copy.start()
        issue(i + ahead)

    def far(i):
        for copy in onward(i):
            copy.wait_recv()

    scale_copies = [
        remote(sc_ref, sc_in.at[s], send_sc.at[s], recv_sc.at[s], device)
        for s, device in enumerate((to_x, to_y, to_d))
    ]
    x_copy = remote(x_ref, x_in, send_a.at[0], recv_a.at[0], to_pair)
    loads[0].wait()
    loads[1].wait()
    wm_ref[:, :mixer_channels] = wm_wide[0].astype(BF16)
    wm_ref[:, mixer_channels:] = wm_wide[1].astype(BF16)
    x_copy.start()
    for copy in scale_copies:
        copy.start()
    issue(0)
    issue(1)
    loads[2].wait()
    wb_ref[...] = wb_wide[...].astype(BF16)
    loads[3].wait()
    loads[4].wait()

    def round_ffn(i, carry):
        rows = pl.ds(pl.multiple_of(i * 64, 64), 64)
        wg_ref[rows, :] = jnp.concatenate(
            (chosen(wg_wide[0, rows, :]), chosen(wg_wide[1, rows, :])), axis=1
        ).astype(BF16)
        return carry

    lax.fori_loop(0, width // 64, round_ffn, 0)
    loads[5].wait()
    wc_ref[...] = wc_wide[...].astype(BF16)

    def feature(s):
        return pl.ds(pl.multiple_of(seat[s] * width, width), width)

    def norm_tile(load, gain, row, size):
        values = [load(s, row).astype(F32) for s in range(4)]
        total = sum(jnp.sum(v * v, axis=1, keepdims=True) for v in values)
        inverse = lax.rsqrt(total / (4 * width) + epsilon)
        for s in range(4):
            xn[s, pl.ds(row, size), :] = (values[s] * inverse * gain[:, feature(s)]).astype(BF16)

    tile = 64

    def norm_own(i, carry):
        norm_tile(lambda s, row: x_ref[pl.ds(row, tile), feature(s)], gain_ref, i * tile, tile)
        return carry

    lax.fori_loop(0, steps // tile, norm_own, 0)
    step(0, 2)
    step(1, 2)
    x_copy.wait_recv()

    def norm_pair(i, carry):
        norm_tile(
            lambda s, row: x_in[pl.ds(i * tile, tile), feature(s)],
            gain_ref, steps + i * tile, tile,
        )
        return carry

    lax.fori_loop(0, steps // tile, norm_pair, 0)
    far(0)
    far(1)

    half = 256
    mixer_in = (wm_ref, wm_in.at[0], wm_in.at[1], wm_in.at[2])

    def mixer_rows(i, carry):
        rows = pl.ds(pl.multiple_of(i * half, half), half)
        plain = dot(xn[0, rows, :], mixer_in[0][...])
        for s in range(1, 4):
            plain += dot(xn[s, rows, :], mixer_in[s][...])
        column_scales = jnp.concatenate(
            (product_scale_ref[:, shard], placewise_scale_ref[:, shard]), axis=1
        )
        both = jax.nn.gelu(plain * column_scales)
        carrier[rows, :] = both[:, :mixer_channels]
        own_spread = both[:, mixer_channels:]
        spread[rows, :] = own_spread
        total = jnp.sum(own_spread * own_spread, axis=1, keepdims=True)
        sums[0, :, rows] = jnp.broadcast_to(total, (half, 128)).T[:8]
        return carry

    lax.fori_loop(0, tokens // half, mixer_rows, 0)
    core_sums = remote(sums.at[0], sums_in.at[0], send_a.at[1], recv_a.at[1], to_core)
    core_sums.start()
    core_sums.wait_recv()
    sums[1] = sums[0] + sums_in[0]
    pair_sums = remote(sums.at[1], sums_in.at[1], send_a.at[2], recv_a.at[2], to_pair)
    pair_sums.start()
    step(2, 2)
    issue(5)
    pair_sums.wait_recv()
    received = sums_in[1]
    received = jnp.concatenate((received[:, steps:], received[:, :steps]), axis=1)
    sums[2] = lax.rsqrt((sums[1] + received) / all_channels + epsilon)

    causal = lax.broadcasted_iota(jnp.int32, (BLOCK, BLOCK), 0) >= lax.broadcasted_iota(
        jnp.int32, (BLOCK, BLOCK), 1
    )
    groups = mixer_channels // GROUP_DIM
    first_group = (2 * k + h) * groups

    def mix_rows(i, carry):
        rows = pl.ds(pl.multiple_of(i * BLOCK, BLOCK), BLOCK)
        factor = jnp.concatenate([sums[2, :, rows]] * (128 // 8), axis=0).T[:, :1]
        normed = (spread[rows, :] * factor * rescale_ref[:, shard]).astype(BF16)
        for g in range(groups):
            lanes = pl.ds(g * GROUP_DIM, GROUP_DIM)
            operator = place_ref[first_group + g]
            operator = jnp.where(causal, operator, jnp.zeros_like(operator))
            offset = jnp.broadcast_to(bias_ref[pl.ds(first_group + g, 1), :], (BLOCK, BLOCK)).T
            mixed = dot(operator, normed[:, g * GROUP_DIM : (g + 1) * GROUP_DIM])
            mixed = mixed + offset
            gated[rows, lanes] = (carrier[rows, lanes] * mixed).astype(BF16)
        return carry

    lax.fori_loop(0, tokens // BLOCK, mix_rows, 0)
    for copy in scale_copies:
        copy.wait_recv()
    scales = (sc_ref, sc_in.at[0], sc_in.at[1], sc_in.at[2])
    keep = (k + fy) % 2
    base = 2 * keep

    def project(values, weights, row, s, target):
        def rows_of(i, carry):
            rows = pl.ds(pl.multiple_of(i * half, half), half)
            target[s, rows, :] = (
                dot(values[rows, :], weights[...]) * scales[s][row : row + 1, :]
            ).astype(BF16)
            return carry

        lax.fori_loop(0, tokens // half, rows_of, 0)

    mixer_out = (wb_ref, wb_in.at[0], wb_in.at[1], wb_in.at[2])
    ffn_out = (wc_ref, wc_in.at[0], wc_in.at[1], wc_in.at[2])

    give = pl.ds(2 - base, 2)
    mix_give = remote(parts.at[give], core_in, send_a.at[3], recv_a.at[3], to_core)
    mix_pair = [
        remote(pair_out.at[j], pair_in.at[j], send_a.at[4 + j], recv_a.at[4 + j], to_pair)
        for j in range(2)
    ]

    def merge_mix():
        mix_give.wait_recv()
        for j in range(2):
            def rows_of(i, carry):
                rows = pl.ds(pl.multiple_of(i * half, half), half)
                pair_out[j, rows, :] = (
                    parts[base + j, rows, :].astype(F32) + core_in[j, rows, :].astype(F32)
                ).astype(BF16)
                return carry

            lax.fori_loop(0, tokens // half, rows_of, 0)
            mix_pair[j].start()

    for t in range(2):
        if t == 1:
            far(2)
        for s in (2 * t, 2 * t + 1):
            project(gated, mixer_out[s], 0, s, parts)

        @pl.when(keep != t)
        def _():
            mix_give.start()

        @pl.when(keep == t)
        def _():
            merge_mix()

    step(3, 3)
    step(4, len(pieces))

    stream_give = [
        remote(stream.at[base + j], stream.at[base + j], send_a.at[6 + j], recv_a.at[6 + j], to_core)
        for j in range(2)
    ]
    stream_take = [
        remote(stream.at[2 - base + j], stream.at[2 - base + j], send_a.at[6 + j], recv_a.at[6 + j], to_core)
        for j in range(2)
    ]
    block_of = (seat[0] + keep * (seat[2] - seat[0]), seat[1] + keep * (seat[3] - seat[1]))
    for j in range(2):
        mix_pair[j].wait_recv()
        lanes = pl.ds(pl.multiple_of(block_of[j] * width, width), width)
        for first, second, source in ((0, steps, x_ref), (steps, 0, x_in)):
            rows = pl.ds(first, steps)
            stream[base + j, rows, :] = (
                source[:, lanes].astype(F32)
                + (
                    pair_out[j, rows, :].astype(F32)
                    + pair_in[j, pl.ds(second, steps), :].astype(F32)
                )
            ).astype(BF16)
        stream_give[j].start()
    for copy in stream_take:
        copy.wait_recv()

    def norm_stream(i, carry):
        norm_tile(
            lambda s, row: stream[s, pl.ds(row, tile), :], ffn_gain_ref, i * tile, tile
        )
        return carry

    lax.fori_loop(0, tokens // tile, norm_stream, 0)
    step(5, 2)
    step(6, 2)
    for i in range(3, 7):
        far(i)

    ffn_in = (wg_ref, wg_in.at[0], wg_in.at[1], wg_in.at[2])

    def ffn_rows(i, carry):
        rows = pl.ds(pl.multiple_of(i * half, half), half)
        plain = dot(xn[0, rows, :], ffn_in[0][...])
        for s in range(1, 4):
            plain += dot(xn[s, rows, :], ffn_in[s][...])
        plain = plain * jnp.concatenate(
            (
                chosen(switch_scale_ref[...][None]),
                chosen(expand_scale_ref[...][None]),
            ), axis=1
        )
        active[rows, :] = (jax.nn.silu(plain[:, :hidden]) * plain[:, hidden:]).astype(BF16)
        return carry

    lax.fori_loop(0, tokens // half, ffn_rows, 0)
    step(7, 2)
    step(8, 2)

    ffn_give = [
        remote(ffn_parts.at[2 - base + j], ffn_core_in.at[j], send_a.at[i], recv_a.at[i], to_core)
        for j, i in enumerate((8, 11))
    ]
    ffn_pair = [
        remote(ffn_pair_out.at[j], ffn_pair_in.at[j], send_a.at[9 + j], recv_a.at[9 + j], to_pair)
        for j in range(2)
    ]

    def merge_ffn(j):
        ffn_give[j].wait_recv()
        rows = pl.ds(steps, steps)
        ffn_pair_out[j] = (
            ffn_parts[base + j, rows, :].astype(F32) + ffn_core_in[j, rows, :].astype(F32)
        ).astype(BF16)
        ffn_pair[j].start()

    for s in range(4):
        t, j = s // 2, s % 2
        if s == 3:
            far(7)
            far(8)
        project(active, ffn_out[s], 1, s, ffn_parts)

        @pl.when(keep != t)
        def _():
            ffn_give[j].start()

        @pl.when(keep == t)
        def _():
            merge_ffn(j)

    own_rows = pl.ds(0, steps)
    for j in range(2):
        ffn_pair[j].wait_recv()
        column = fx + j - 2 * fx * j
        lanes = pl.ds(pl.multiple_of(column * width, width), width)
        out_ref[:, lanes] = (
            stream[base + j, own_rows, :].astype(F32)
            + (
                ffn_parts[base + j, own_rows, :].astype(F32)
                + ffn_core_in[j, own_rows, :].astype(F32)
                + ffn_pair_in[j].astype(F32)
            )
        ).astype(BF16)

    for i in range(len(pieces)):
        for copy in own(i) + onward(i):
            copy.wait_send()
    for copy in scale_copies + [x_copy, core_sums, pair_sums, mix_give] + ffn_give:
        copy.wait_send()
    for copy in mix_pair + stream_give + ffn_pair:
        copy.wait_send()


def in_one_kernel(

    skip_stream_entry,
    sequence_blender_factor,
    product_projector,
    product_side_factors,
    placewise_projector,
    placewise_entry_factors,
    placewise_rescale_factor,
    place_cluster_operator,
    placewise_offset_vector,
    blender_result_projector,
    blender_result_factors,
    feedforward_norm_factor,
    switch_projector,
    switch_factors,
    expand_projector,
    expand_factors,
    contract_projector,
    contract_factors,
):
    steps, embed = skip_stream_entry.shape
    tokens = 2 * steps
    width = product_projector.shape[0]
    channels = product_projector.shape[1] // 2
    hidden = switch_projector.shape[1] // 2

    vmem = pltpu.VMEM
    dma = pltpu.SemaphoreType.DMA
    blocks = (4, tokens, width)
    two = (2, tokens, width)
    return pl.pallas_call(
        functools.partial(
            layer_kernel,
            mixer_channels=channels,
            all_channels=2 * channels * lax.axis_size("tp"),
        ),
        out_shape=jax.ShapeDtypeStruct((steps, embed // 2), BF16),
        in_specs=[pl.BlockSpec(memory_space=vmem)]
        + [pl.BlockSpec(memory_space=pl.ANY)] * 6
        + [pl.BlockSpec(memory_space=vmem)] * 11,
        out_specs=pl.BlockSpec(memory_space=vmem),
        scratch_shapes=[
            vmem((width, 2 * channels), BF16),
            vmem((channels, width), BF16),
            vmem((width, 2 * hidden), BF16),
            vmem((hidden, width), BF16),
            vmem((8, width), F32),
            vmem((2, width, channels), F32),
            vmem((channels, width), F32),
            vmem((2, width, 2 * hidden), F32),
            vmem((hidden, width), F32),
            vmem((3, width, 2 * channels), BF16),
            vmem((3, channels, width), BF16),
            vmem((3, width, 2 * hidden), BF16),
            vmem((3, hidden, width), BF16),
            vmem((3, 8, width), F32),
            vmem((steps, embed), BF16),
            vmem(blocks, BF16),
            vmem((tokens, channels), F32),
            vmem((tokens, channels), F32),
            vmem((tokens, channels), BF16),
            vmem((3, 8, tokens), F32),
            vmem((2, 8, tokens), F32),
            vmem(blocks, BF16),
            vmem(two, BF16),
            vmem(two, BF16),
            vmem(two, BF16),
            vmem(blocks, BF16),
            vmem((tokens, hidden), BF16),
            vmem(blocks, BF16),
            vmem(two, BF16),
            vmem((2, steps, width), BF16),
            vmem((2, steps, width), BF16),
            dma((9, 4)),
            dma((9, 4)),
            dma((3,)),
            dma((3,)),
            dma((12,)),
            dma((12,)),
            dma((6,)),
        ],
        compiler_params=pltpu.CompilerParams(
            collective_id=0, has_side_effects=True, vmem_limit_bytes=60 * 1024 * 1024
        ),
    )(
        skip_stream_entry,
        product_projector,
        placewise_projector,
        blender_result_projector,
        switch_projector,
        expand_projector,
        contract_projector,
        sequence_blender_factor[None],
        feedforward_norm_factor[None],
        product_side_factors[None],
        placewise_entry_factors[None],
        placewise_rescale_factor[None],
        switch_factors,
        expand_factors,
        blender_result_factors[None],
        contract_factors[None],
        place_cluster_operator,
        placewise_offset_vector,
    )


def on_device(*arrays):
    entry, mixer, switch = arrays[0], arrays[2], arrays[12]
    fits = (
        lax.axis_size("rep") % 2 == 0
        and lax.axis_size("fs") == 4
        and lax.axis_size("tp") == 2
        and entry.shape[0] % 256 == 0
        and mixer.shape[0] % 128 == 0
        and mixer.shape[1] % (2 * GROUP_DIM) == 0
        and switch.shape[1] % 128 == 0
    )
    return in_one_kernel(*arrays) if fits else with_collectives(*arrays)


def solution(mesh):
    return jax.shard_map(
        on_device,
        mesh=mesh,
        in_specs=(
            P(("rep", "fs"), None),
            P(),
            P("fs", "tp"),
            P("tp"),
            P("fs", "tp"),
            P("tp"),
            P("tp"),
            P(),
            P(),
            P("tp", "fs"),
            P("fs"),
            P(),
            P("fs", "tp"),
            P("tp"),
            P("fs", "tp"),
            P("tp"),
            P("tp", "fs"),
            P("fs"),
        ),
        out_specs=P(("rep", "fs"), "tp"),
        check_vma=False,
    )
```
